32 devices in a mesh: sp: 16 (over z, y, x), tp: 2 (over core).
Axes of the slice: x: 2, y: 2, z: 4, core: 2. Of those that a mesh axis runs over, the one named last changes fastest.
Arguments:
- residual: bfloat16 [4096, 2048], P('sp'), may hold values from -6 to 6
- queries: bfloat16 [4096, 1024], P('sp', 'tp'), may hold values from -6 to 6
- forget_gate_logits: bfloat16 [4096, 1024], P('sp', 'tp'), may hold values from -5 to 5
- projected_values: bfloat16 [4096, 1024], P('sp', 'tp'), may hold values from -6 to 6
- output_gate_logits: bfloat16 [4096, 1024], P('sp', 'tp'), may hold values from -6 to 6
- lower_bound_margin: float32 [1024], P('tp'), may hold values from 0.00024414062 to 0.08
- extra_forget_logs: float32 [4096, 1024], P('sp', 'tp'), may hold values from -0.7 to 0
- per_head_norm_gain: float32 [128], replicated, may hold values from 0.1 to 1.9
- output_weight: bfloat16 [1024, 2048], P('tp'), may hold values from -0.1875 to 0.1875
- feedforward_norm_gain: float32 [2048], replicated, may hold values from 0.1 to 1.9
- gate_weight: bfloat16 [2048, 5632], P('sp', 'tp'), may hold values from -0.125 to 0.125
- up_weight: bfloat16 [2048, 5632], P('sp', 'tp'), may hold values from -0.125 to 0.125
- down_weight: bfloat16 [5632, 2048], P('tp', 'sp'), may hold values from -0.078125 to 0.078125
Outputs:
- layer_out: bfloat16 [4096, 2048], P('sp')
The draws below stay inside these ranges and needn't reach their ends.
All inputs are finite; a program needn't handle non-finite values.
Results may differ from the reference program's by a relative error of at most 0.015.
Values may be sent and summed in bfloat16 or wider, within the bound.
A program may use at most 128 MiB of HBM per device.

```python
import math
import jax
import jax.numpy as jnp
from jax import lax

D = 2048
FF = 5632
HEADS = 8
HD = 128
HW = 1024
BLOCK = 64
TOK_DEV = 256
SEQ = 4096
N_TP = 2


def draw_lower_bound_margin(key, part):
    order = jax.random.permutation(jax.random.fold_in(key, 1), HEADS)
    slow = order < HEADS // 2
    slow_gap = 2.0 / SEQ * jax.random.uniform(jax.random.fold_in(key, 2), (HEADS, HD), jnp.float32, 0.5, 1.5)
    fast_gap = jnp.exp(jax.random.uniform(jax.random.fold_in(key, 3), (HEADS, HD), jnp.float32, math.log(0.03), math.log(0.08)))
    gaps = jnp.where(slow[:, None], slow_gap, fast_gap)
    return gaps.reshape(HW).astype(jnp.float32)


def draw_forget_gate_logits(key, part):
    base = jnp.clip(jax.random.normal(jax.random.fold_in(key, 1), (SEQ, HW), jnp.float32), -4.0, 4.0)
    shifts = jax.random.uniform(jax.random.fold_in(key, 2), (SEQ // TOK_DEV, 1, HW), jnp.float32, -1.0, 1.0)
    shifted = base.reshape(SEQ // TOK_DEV, TOK_DEV, HW) + shifts
    return shifted.reshape(SEQ, HW).astype(jnp.bfloat16)


def draw_extra_forget_logs(key, part):
    spots = jax.random.randint(jax.random.fold_in(key, 1), (4,), 0, SEQ)
    struck = jnp.any(jnp.arange(SEQ)[:, None] == spots[None, :], axis=1)
    depth = jax.random.uniform(jax.random.fold_in(key, 2), (SEQ, HW), jnp.float32, math.log(0.5), math.log(0.8))
    return jnp.where(struck[:, None], depth, 0.0).astype(jnp.float32)


def steps_of(stream_key, shape, cuts, least, largest):
    gain, own = 1.0, jax.random.fold_in(stream_key, 6)
    for axis_at, blocks in cuts:
        draws = jnp.exp(jax.random.uniform(jax.random.fold_in(own, axis_at), (blocks,), jnp.float32, least / len(cuts), largest / len(cuts)))
        gain = gain * jnp.repeat(draws, shape[axis_at] // blocks).reshape([-1 if axis == axis_at else 1 for axis in range(len(shape))])
    return gain


def centred(stream_key, shape, scale, limit, shards=(), kind=jnp.bfloat16):
    loudness = steps_of(stream_key, shape, shards, -0.22, 0.18) if shards else 1.0
    values = jax.random.normal(stream_key, shape, jnp.float32) * scale * loudness
    return jnp.minimum(jnp.maximum(values, -limit), limit).astype(kind)


def setup_inputs(seed: int = 0) -> dict:
    arg_keys = jax.random.split(jax.random.key(seed), 14)
    return {
        "residual": centred(arg_keys[0], (SEQ, D), 1.0, 6.0, ((0, 16),)),
        "queries": centred(arg_keys[1], (SEQ, HW), 1.0, 6.0, ((0, 16), (1, 2))),
        "forget_gate_logits": draw_forget_gate_logits(jax.random.fold_in(arg_keys[13], 71), 0),
        "projected_values": centred(arg_keys[3], (SEQ, HW), 1.0, 6.0, ((0, 16), (1, 2))),
        "output_gate_logits": centred(arg_keys[4], (SEQ, HW), 1.0, 6.0, ((0, 16), (1, 2))),
        "lower_bound_margin": draw_lower_bound_margin(jax.random.fold_in(arg_keys[13], 71), 0),
        "extra_forget_logs": draw_extra_forget_logs(jax.random.fold_in(arg_keys[13], 71), 0),
        "per_head_norm_gain": jnp.clip(1.0 + 0.18 * jax.random.normal(arg_keys[7], (HD,), jnp.float32), 0.1, 1.9),
        "output_weight": centred(arg_keys[8], (HW, D), HW ** -0.5, 0.1875, ((0, 2),)),
        "feedforward_norm_gain": jnp.clip(1.0 + 0.18 * jax.random.normal(arg_keys[9], (D,), jnp.float32), 0.1, 1.9),
        "gate_weight": centred(arg_keys[10], (D, FF), D ** -0.5, 0.125, ((0, 16), (1, 2))),
        "up_weight": centred(arg_keys[11], (D, FF), D ** -0.5, 0.125, ((0, 16), (1, 2))),
        "down_weight": centred(arg_keys[12], (FF, D), FF ** -0.5, 0.078125, ((0, 2), (1, 16))),
    }


eps = 1e-06
top_precision = lax.Precision.HIGHEST

def block_update(recurrent_state, inputs):
    queries, state_increment, value_rows, retain_log_factor = inputs
    running_state = jnp.cumsum(retain_log_factor, axis=1)
    causal = jnp.tril(jnp.ones((retain_log_factor.shape[1], retain_log_factor.shape[1]), dtype=bool))
    carried_over_state = jnp.einsum('uqw,uwa->uqa', queries * jnp.exp(running_state), recurrent_state, precision=top_precision)
    spread = running_state[:, :, None, :] - running_state[:, None, :, :]
    weights = jnp.exp(jnp.where(causal[None, :, :, None], spread, -jnp.inf))
    scores = jnp.einsum('htk,htsk,hsk->hts', queries, weights, state_increment, precision=top_precision)
    output_rows = carried_over_state + jnp.einsum('hts,hsv->htv', scores, value_rows, precision=top_precision)
    final_state = running_state[:, -1:, :]
    updated_state = jnp.exp(final_state[:, 0, :])[:, :, None] * recurrent_state + jnp.einsum('erb,erc->ebc', state_increment * jnp.exp(final_state - running_state), value_rows, precision=top_precision)
    return (updated_state, output_rows)

def grouped_product(left, right, groups):
    group_width = left.shape[1] // groups
    summed = jnp.zeros((left.shape[0], right.shape[1]), jnp.float32)
    for member in range(groups):
        lower = member * group_width
        upper = lower + group_width
        part_product = jnp.dot(left[:, lower:upper], right[lower:upper], preferred_element_type=jnp.float32)
        rounded = lax.optimization_barrier(part_product.astype(jnp.bfloat16))
        summed = summed + rounded.astype(jnp.float32)
    return summed

def reference(residual, queries, forget_gate_logits, projected_values, output_gate_logits, lower_bound_margin, extra_forget_logs, per_head_norm_gain, output_weight, feedforward_norm_gain, gate_weight, up_weight, down_weight):
    state_increment = lower_bound_margin * jax.nn.sigmoid(-forget_gate_logits.astype(jnp.float32))
    retain_log_factor = jnp.log1p(-state_increment) + extra_forget_logs

    def to_blocks(source):
        return source.reshape(SEQ // BLOCK, BLOCK, HEADS, HD).transpose(0, 2, 1, 3)
    initial = jnp.zeros((HEADS, HD, HD), jnp.float32)
    block_inputs = (to_blocks(queries.astype(jnp.float32)), to_blocks(state_increment), to_blocks(projected_values.astype(jnp.float32)), to_blocks(retain_log_factor))
    _, output_rows = lax.scan(block_update, initial, block_inputs)
    mixed = output_rows.transpose(0, 2, 1, 3).reshape(SEQ, HEADS, HD)
    normed_heads = mixed * lax.rsqrt(lax.optimization_barrier(jnp.mean(mixed * mixed, axis=-1, keepdims=True)) + eps) * per_head_norm_gain
    gating = jax.nn.silu(output_gate_logits.astype(jnp.float32)).reshape(SEQ, HEADS, HD)
    gated = (normed_heads * gating).reshape(SEQ, HW).astype(jnp.bfloat16)
    projected = grouped_product(gated, output_weight, N_TP)
    after_mixer = (residual.astype(jnp.float32) + projected).astype(jnp.bfloat16)
    widened = after_mixer.astype(jnp.float32)
    normed = (widened * lax.rsqrt(lax.optimization_barrier(jnp.mean(widened * widened, axis=-1, keepdims=True)) + eps) * feedforward_norm_gain).astype(jnp.bfloat16)
    group_width = FF // N_TP
    ffn_sum = jnp.zeros((SEQ, D), jnp.float32)
    for member in range(N_TP):
        lower = member * group_width
        upper = lower + group_width
        gate_part = jnp.dot(normed, gate_weight[:, lower:upper], preferred_element_type=jnp.float32)
        up_part = jnp.dot(normed, up_weight[:, lower:upper], preferred_element_type=jnp.float32)
        hidden = (jax.nn.silu(gate_part) * up_part).astype(jnp.bfloat16)
        part_product = jnp.dot(hidden, down_weight[lower:upper], preferred_element_type=jnp.float32)
        rounded = lax.optimization_barrier(part_product.astype(jnp.bfloat16))
        ffn_sum = ffn_sum + rounded.astype(jnp.float32)
    return (after_mixer.astype(jnp.float32) + 0.5 * ffn_sum).astype(jnp.bfloat16)
```

```python
import jax
import jax.numpy as jnp
from jax import lax
from jax.experimental import pallas as pl
from jax.experimental.pallas import tpu as pltpu
from jax.sharding import PartitionSpec as P

HD = 128
BLOCK = 64


eps = 1e-06
top_precision = lax.Precision.HIGHEST


def carried_in_2(value, axis, join, neutral):
    place = lax.axis_index(axis)
    gathered = jax.tree.map(
        lambda a, kind: lax.all_gather(a.astype(kind), axis), value, (jnp.bfloat16, jnp.bfloat16)
    )
    state = jax.tree.map(lambda a, e: jnp.zeros_like(a) + jnp.asarray(e, a.dtype), value, neutral)

    def one(turn, state):
        return join(
            state,
            jax.tree.map(
                lambda a, own: lax.dynamic_index_in_dim(a, turn, 0, False).astype(own.dtype),
                gathered,
                value,
            ),
        )

    return lax.fori_loop(0, place, one, state)


def block_update(carried_in, inputs):
    recurrent_state, offset = carried_in
    queries, state_increment, value_rows, retain_log_factor = inputs
    running_state = jnp.cumsum(retain_log_factor, axis=1)
    causal = jnp.tril(
        jnp.ones((retain_log_factor.shape[1], retain_log_factor.shape[1]), dtype=bool)
    )
    carried_over_state = jnp.einsum(
        "uqw,uwa->uqa", queries * jnp.exp(running_state), recurrent_state, precision=top_precision
    )
    spread = running_state[:, :, None, :] - running_state[:, None, :, :]
    weights = jnp.exp(jnp.where(causal[None, :, :, None], spread, -jnp.inf))
    scores = jnp.einsum(
        "htk,htsk,hsk->hts", queries, weights, state_increment, precision=top_precision
    )
    output_rows = carried_over_state + jnp.einsum(
        "hts,hsv->htv", scores, value_rows, precision=top_precision
    )
    final_state = running_state[:, -1:, :]
    updated_state = jnp.exp(final_state[:, 0, :])[:, :, None] * recurrent_state + jnp.einsum(
        "erb,erc->ebc",
        state_increment * jnp.exp(final_state - running_state),
        value_rows,
        precision=top_precision,
    )
    rescaled_state = queries * jnp.exp(running_state + offset[:, None, :])
    return ((updated_state, offset + final_state[:, 0, :]), (output_rows, rescaled_state))


def join_states(earlier, later):
    earlier_sum, earlier_memory = earlier
    later_sum, later_memory = later
    return (earlier_sum + later_sum, jnp.exp(later_sum)[:, :, None] * earlier_memory + later_memory)


MESH = pl.DeviceIdType.MESH
GROUPS = 4


def up_to(value, step):
    return -(-value // step) * step


def layer_kernel(
    dims, gate_hbm, up_hbm, dn_ref, q_hbm, f_hbm, v_hbm, og_hbm, extra_hbm, ow_hbm, res_hbm,
    margin_ref, head_gain_ref, ff_gain_ref, out_ref,
    gate_in, up_in, q_ref, f_ref, v_ref, og_ref, extra_ref, ow_ref, residual,
    gu_own, gu, dn, grown, q_grown, st_out, st_in, tot_out, tot_in, inc_out, inc,
    gated, proj, proj_got, x_own, rows_in, hid, part, peer_part, summed, xgot, pair, zgot,
    s_l, s_a, r_a, s_b, r_b, s_1, r_1, s_2, r_2, s_3, r_3, s_j, r_j, s_x, r_x, s_p, r_p,
    s_d, r_d, s_r, r_r, s_z, r_z, s_o, r_o,
):
    share, own, width, padded = dims
    me = lax.axis_index("sp")
    c = lax.axis_index("tp")
    z, r = me // 4, me % 4
    zh, zl, y, x = z // 2, z % 2, r // 2, r % 2
    inner = (zh + zl) % 2 == 1
    model = gu.shape[0]
    half = share // 2
    bf, f32 = jnp.bfloat16, jnp.float32

    def flip(value, d):
        return (value + d) % 2

    def place(o, dy=0):
        return (flip(zh, o // 4) * 2 + flip(zl, o // 2 % 2)) * 4 + flip(y, dy) * 2 + flip(x, o % 2)

    def group(o):
        return flip(x, o % 2) * 2 + flip(zl, o // 2 % 2)

    def beside(e):
        return flip(y, e // 2) * 2 + flip(x, e % 2)

    def remote(src, dst, send, recv, to, core):
        return pltpu.make_async_remote_copy(
            src_ref=src, dst_ref=dst, send_sem=send, recv_sem=recv, device_id=(to, core), device_id_type=MESH,
        )

    sent = []

    def go(copy):
        copy.start()
        sent.append(copy)
        return copy

    barrier = pltpu.get_barrier_semaphore()
    partners = [(place(o), c) for o in range(1, 8)] + [(place(0, 1), c), (place(1, 1), c), (me, 1 - c)]
    for partner in partners:
        pl.semaphore_signal(barrier, inc=1, device_id=partner, device_id_type=MESH)

    mine = pl.ds(pl.multiple_of(c * own, own), own)
    theirs = pl.ds(pl.multiple_of((1 - c) * own, own), own)
    loads = [
        pltpu.make_async_copy(src, dst, s_l.at[i])
        for i, (src, dst) in enumerate((
            (gate_hbm, gate_in), (up_hbm, up_in), (q_hbm, q_ref), (f_hbm, f_ref), (v_hbm, v_ref),
            (extra_hbm, extra_ref), (og_hbm, og_ref), (ow_hbm, ow_ref), (res_hbm.at[mine], residual),
            (dn_ref.at[group(0)], dn.at[pl.ds(0, width), pl.ds(pl.multiple_of(me * share, share), share)]),
        ))
    ]
    for load in loads:
        load.start()

    def region(owner, k):
        if k < 2:
            return gu.at[pl.ds(pl.multiple_of(owner * share + k * half, half), half)]
        return dn.at[pl.ds(0, width), pl.ds(pl.multiple_of(owner * share, share), share)]

    def origin(g, k):
        return gu_own.at[g, pl.ds(k * half, half)] if k < 2 else dn_ref.at[g]

    def direct(o, k):
        return remote(origin(group(o), k), region(me, k), s_a.at[o, k], r_a.at[o, k], place(o), c)

    def lend(o, k):
        block = region(place(o), k)
        return remote(origin(group(0), k) if o == 0 else block, block, s_b.at[o, k], r_b.at[o, k], place(0, 1), c)

    def send(*pieces):
        for o, k in pieces:
            direct(o, k).start()

    def relay(*pieces):
        for o, k in pieces:
            if o:
                direct(o, k).wait_recv()
            lend(o, k).start()

    loads[0].wait()
    loads[1].wait()
    even = width // 128 * 128
    for g in range(GROUPS):
        first = g * width
        gate, up = gate_in[:, first:first + width], up_in[:, first:first + width]
        for at in range(0, even, 128):
            gu_own[g, :, 2 * at:2 * at + 128] = gate[:, at:at + 128]
            gu_own[g, :, 2 * at + 128:2 * at + 256] = up[:, at:at + 128]
        if width > even:
            gu_own[g, :, 2 * even:] = jnp.concatenate([gate[:, even:], up[:, even:]], axis=1)
    gu[pl.ds(pl.multiple_of(me * share, share), share), :] = gu_own[group(0)]
    if padded > width:
        dn[pl.ds(width, padded - width), :] = jnp.zeros((padded - width, model), dn.dtype)

    pl.semaphore_wait(barrier, len(partners))

    @pl.when(inner)
    def _():
        send((4, 0), (6, 0))

    send((2, 0), (1, 0))
    relay((0, 0))

    length, channels = q_ref.shape
    heads = channels // HD
    span = 128
    ones = lambda n: lax.broadcasted_iota(jnp.int32, (n, n), 0) >= lax.broadcasted_iota(jnp.int32, (n, n), 1)
    lower = ones(length).astype(f32)
    causal = ones(span)
    over = lambda p, q, i, j: lax.dot_general(p, q, (((i,), (j,)), ((), ())), preferred_element_type=f32)

    def logs_tile(logs):
        high = logs.astype(bf)
        low = (logs - high.astype(f32)).astype(bf)
        return jnp.concatenate([jnp.broadcast_to(high, (8, HD)), jnp.broadcast_to(low, (8, HD))], axis=0)

    def part_of(ref, at):
        tile = ref[at, HD:HD + 16, :].astype(f32)
        return tile[0:1] + tile[8:9], ref[at, 0:HD, :].astype(f32)

    for i in range(2, 6):
        loads[i].wait()
    for n in range(heads):
        cols = slice(n * HD, (n + 1) * HD)
        inflow = margin_ref[:, cols] * jax.nn.sigmoid(-f_ref[:, cols].astype(f32))
        keep = jnp.log1p(-inflow) + extra_ref[:, cols]
        total_log = lax.dot_general(lower, keep, (((1,), (0,)), ((), ())), precision=top_precision, preferred_element_type=f32)
        q = q_ref[:, cols].astype(f32)
        q_grown[:, cols] = (q * jnp.exp(total_log)).astype(bf)
        state = None
        for start in range(0, length, span):
            rows = slice(start, start + span)
            a, qb, ub, vb = total_log[rows], q[rows], inflow[rows], v_ref[rows, cols]
            middle, end = a[span // 2 - 1:span // 2], a[span - 1:span]
            scores = over((qb * jnp.exp(a - middle)).astype(bf), (ub * jnp.exp(middle - a)).astype(bf), 1, 1)
            mixed = over(jnp.where(causal, scores, 0.0).astype(bf), vb, 1, 0)
            added = over(vb, (ub * jnp.exp(end - a)).astype(bf), 0, 0)
            if state is None:
                state = added
            else:
                mixed = mixed + over((qb * jnp.exp(a - base)).astype(bf), state.astype(bf), 1, 1)
                state = state * jnp.exp(end - base) + added
            grown[rows, cols] = mixed
            base = end
        st_out[n, 0:HD, :] = state.astype(bf)
        st_out[n, HD:HD + 16, :] = logs_tile(base)

    to_head = [
        go(remote(st_out.at[beside(e)], st_in.at[r], s_1.at[e - 1], r_1.at[e - 1], z * 4 + beside(e), c)) for e in (3, 1, 2)
    ]
    st_in[r] = st_out[r]
    send((1, 1))
    relay((0, 1), (0, 2))
    for copy in to_head:
        copy.wait_recv()
    whole, whole_log, before = jnp.zeros((HD, HD), f32), jnp.zeros((1, HD), f32), []
    for at in range(4):
        logs, state = part_of(st_in, at)
        before.append((whole_log, whole))
        whole = whole * jnp.exp(logs) + state
        whole_log = whole_log + logs
    tot_out[0, 0:HD, :] = whole.astype(bf)
    tot_out[0, HD:HD + 16, :] = logs_tile(whole_log)
    along = [go(remote(tot_out.at[0], tot_in.at[z], s_2.at[d - 1], r_2.at[d - 1], place(2 * d), c)) for d in (2, 3, 1)]

    @pl.when(inner)
    def _():
        send((4, 1), (6, 1), (4, 2))

    @pl.when(jnp.logical_not(inner))
    def _():
        send((4, 0), (6, 0), (4, 1))

    send((1, 2))
    for copy in along:
        copy.wait_recv()
    state = jnp.zeros((HD, HD), f32)
    for at in range(3):
        logs, later = part_of(tot_in, at)
        state = jnp.where(at < z, state * jnp.exp(logs) + later, state)
    for at in range(4):
        early_log, early = before[at]
        inc_out[at] = (state * jnp.exp(early_log) + early).astype(bf)
    to_rows = [
        go(remote(inc_out.at[beside(e)], inc.at[r], s_3.at[e - 1], r_3.at[e - 1], z * 4 + beside(e), c)) for e in (3, 1, 2)
    ]
    inc[r] = inc_out[r]
    send((5, 0), (7, 0))
    relay((1, 0), (2, 0))
    for i in range(6, 9):
        loads[i].wait()
    for copy in to_rows:
        copy.wait_recv()
    for n in range(heads):
        cols = slice(n * HD, (n + 1) * HD)
        mixed = grown[:, cols] + over(q_grown[:, cols], inc[n], 1, 1)
        scale = lax.rsqrt(jnp.mean(mixed * mixed, axis=-1, keepdims=True) + eps)
        gate = og_ref[:, cols].astype(f32)
        gated[:, cols] = (mixed * scale * head_gain_ref[...] * (gate * jax.nn.sigmoid(gate))).astype(bf)

    def project(j, carry):
        at = pl.multiple_of(j * 256, 256)
        proj[:, pl.ds(at, 256)] = jnp.dot(
            gated[...], ow_ref[:, pl.ds(at, 256)], preferred_element_type=f32
        ).astype(bf)
        return carry

    lax.fori_loop(0, model // 256, project, 0)
    joined = go(remote(proj.at[theirs], proj_got, s_j.at[0], r_j.at[0], me, 1 - c))
    relay((1, 1))
    joined.wait_recv()
    after = (residual[...].astype(f32) + (proj[mine, :].astype(f32) + proj_got[...].astype(f32))).astype(bf)
    x_own[...] = after
    wide = after.astype(f32)
    normed = wide * lax.rsqrt(jnp.mean(wide * wide, axis=-1, keepdims=True) + eps) * ff_gain_ref[...]

    def token_rows(o):
        return pl.ds(pl.multiple_of((c * GROUPS + group(o)) * own, own), own)

    rows_in[token_rows(0), :] = normed.astype(bf)

    def rows_to(o, i, to, core):
        block = rows_in.at[token_rows(o)]
        return go(remote(block, block, s_x.at[i], r_x.at[i], to, core))

    def rows_over(o):
        block = rows_in.at[token_rows(o)]
        return go(remote(block, block, s_p.at[o], r_p.at[o], me, 1 - c))

    to_x, to_z = rows_to(0, 0, place(1), c), rows_to(0, 1, place(2), c)
    peers = [rows_over(0)]

    @pl.when(inner)
    def _():
        send((2, 1), (6, 2), (2, 2))

    @pl.when(jnp.logical_not(inner))
    def _():
        send((6, 1), (2, 1), (4, 2), (6, 2), (2, 2))

    send((5, 1), (7, 1))
    relay((4, 0), (6, 0), (4, 1))
    to_z.wait_recv()
    to_x2 = rows_to(2, 2, place(1), c)
    peers.append(rows_over(2))
    send((3, 0), (3, 1), (5, 2), (7, 2), (3, 2))
    to_x.wait_recv()
    peers.append(rows_over(1))
    relay((1, 2), (6, 1), (2, 1), (5, 0), (7, 0), (5, 1), (7, 1))
    to_x2.wait_recv()
    peers.append(rows_over(3))
    relay((3, 0), (3, 1))
    relay((2, 2), (4, 2))
    for copy in peers:
        copy.wait_recv()
    for o in range(8):
        for k in (0, 1):
            lend(o, k).wait_recv()

    block_rows = 4 * own

    def gate_up(m):
        rows = pl.ds(m * block_rows, block_rows)

        def step(j, carry):
            at = pl.multiple_of(j * 256, 256)
            both = jnp.dot(rows_in[rows, :], gu[:, pl.ds(at, 256)], preferred_element_type=f32)
            gate, up = both[:, :128], both[:, 128:]
            hid[rows, pl.ds(pl.multiple_of(j * 128, 128), 128)] = (gate * jax.nn.sigmoid(gate) * up).astype(bf)
            return carry

        lax.fori_loop(0, width // 128, step, 0)
        if width % 128:
            both = jnp.dot(rows_in[rows, :], gu[:, 2 * even:], preferred_element_type=f32)
            hid[rows, even:] = (both * jax.nn.sigmoid(both) * pltpu.roll(both, 64, 1)).astype(bf)

    gate_up(0)
    relay((6, 2))
    gate_up(1)
    loads[9].wait()

    tile = 2 * share
    my_rows = pl.ds(pl.multiple_of(c * block_rows, block_rows), block_rows)
    their_rows = pl.ds(pl.multiple_of((1 - c) * block_rows, block_rows), block_rows)
    row_pair = pl.ds(pl.multiple_of(x * 2 * own, own), 2 * own)
    other_pair = pl.ds(pl.multiple_of((1 - x) * 2 * own, own), 2 * own)
    row_own = pl.ds(pl.multiple_of(zl * own, own), own)
    row_other = pl.ds(pl.multiple_of((1 - zl) * own, own), own)

    def columns(k):
        at = (flip(zh, k // 4) * 2 + k // 2 % 2) * 4 + flip(y, k % 2) * 2
        return pl.ds(pl.multiple_of(at * share, tile), tile)

    def swap(k):
        return remote(part.at[k, their_rows], peer_part.at[k], s_d.at[k], r_d.at[k], me, 1 - c)

    def across_x(k):
        return remote(summed.at[k, other_pair], xgot.at[k], s_r.at[k], r_r.at[k], place(1), c)

    def across_z(k):
        return remote(pair.at[k, row_other], zgot.at[k], s_z.at[k], r_z.at[k], place(2), c)

    def finish(k):
        block = out_ref.at[mine, columns(k)]
        return remote(block, block, s_o.at[k], r_o.at[k], me, 1 - c)

    def down(k):
        for m in range(2):
            rows = pl.ds(m * block_rows, block_rows)
            part[k, rows, :] = jnp.dot(hid[rows, :], dn[:, columns(k)], preferred_element_type=f32).astype(bf)
        swap(k).start()

    def stage_1(k):
        swap(k).wait_recv()
        summed[k] = (part[k, my_rows, :].astype(f32) + peer_part[k].astype(f32)).astype(bf)
        across_x(k).start()

    def stage_2(k):
        across_x(k).wait_recv()
        pair[k] = (summed[k, row_pair, :].astype(f32) + xgot[k].astype(f32)).astype(bf)
        across_z(k).start()

    def stage_3(k):
        across_z(k).wait_recv()
        total = pair[k, row_own, :].astype(f32) + zgot[k].astype(f32)
        out_ref[mine, columns(k)] = (x_own[:, columns(k)].astype(f32) + 0.5 * total).astype(bf)
        finish(k).start()

    order = (0, 2, 1, 3, 4, 6, 5, 7)
    for turn in range(len(order) + 3):
        if turn == 0:
            relay((3, 2))
        if turn == 1:
            relay((5, 2))
        if turn == 2:
            for o in range(4):
                lend(o, 2).wait_recv()
            relay((7, 2))
        if turn == 6:
            for o in range(4, 8):
                lend(o, 2).wait_recv()
        if turn < len(order):
            down(order[turn])
        if 1 <= turn <= len(order):
            stage_1(order[turn - 1])
        if 2 <= turn <= len(order) + 1:
            stage_2(order[turn - 2])
        if turn >= 3:
            stage_3(order[turn - 3])
    for k in range(8):
        finish(k).wait_recv()
    for copy in sent:
        copy.wait_send()
    for o in range(8):
        for k in range(3):
            if o:
                direct(o, k).wait_send()
            lend(o, k).wait_send()
    for k in range(8):
        for copy in (swap(k), across_x(k), across_z(k), finish(k)):
            copy.wait_send()


def layer(
    residual, queries, forget_gate_logits, projected_values, output_gate_logits, lower_bound_margin,
    extra_forget_logs, per_head_norm_gain, output_weight, feedforward_norm_gain, gate_weight, up_weight, down_weight,
):
    share, half = gate_weight.shape
    width = half // GROUPS
    padded = up_to(width, 128)
    length, model = residual.shape
    own = length // 2
    channels = queries.shape[1]
    dn = down_weight.reshape(GROUPS, width, share)
    bf, f32 = jnp.bfloat16, jnp.float32
    dma = pltpu.SemaphoreType.DMA
    dims = (share, own, width, padded)
    vm = pl.BlockSpec(memory_space=pltpu.VMEM)
    hbm = pl.BlockSpec(memory_space=pltpu.HBM)
    message = HD + 16
    tile = 2 * share
    chunks = model // tile
    return pl.pallas_call(
        lambda *refs: layer_kernel(dims, *refs),
        out_shape=jax.ShapeDtypeStruct((length, model), bf),
        in_specs=[hbm] * 10 + [vm] * 3,
        out_specs=vm,
        scratch_shapes=[
            pltpu.VMEM((share, half), bf),
            pltpu.VMEM((share, half), bf),
            pltpu.VMEM((length, channels), bf),
            pltpu.VMEM((length, channels), bf),
            pltpu.VMEM((length, channels), bf),
            pltpu.VMEM((length, channels), bf),
            pltpu.VMEM((length, channels), f32),
            pltpu.VMEM((channels, model), bf),
            pltpu.VMEM((own, model), bf),
            pltpu.VMEM((GROUPS, share, 2 * width), bf),
            pltpu.VMEM((model, 2 * width), bf),
            pltpu.VMEM((padded, model), bf),
            pltpu.VMEM((length, channels), f32),
            pltpu.VMEM((length, channels), bf),
            pltpu.VMEM((4, message, HD), bf),
            pltpu.VMEM((4, message, HD), bf),
            pltpu.VMEM((1, message, HD), bf),
            pltpu.VMEM((4, message, HD), bf),
            pltpu.VMEM((4, HD, HD), bf),
            pltpu.VMEM((4, HD, HD), bf),
            pltpu.VMEM((length, channels), bf),
            pltpu.VMEM((length, model), bf),
            pltpu.VMEM((own, model), bf),
            pltpu.VMEM((own, model), bf),
            pltpu.VMEM((GROUPS * length, model), bf),
            pltpu.VMEM((GROUPS * length, padded), bf),
            pltpu.VMEM((chunks, GROUPS * length, tile), bf),
            pltpu.VMEM((chunks, GROUPS * own, tile), bf),
            pltpu.VMEM((chunks, GROUPS * own, tile), bf),
            pltpu.VMEM((chunks, 2 * own, tile), bf),
            pltpu.VMEM((chunks, 2 * own, tile), bf),
            pltpu.VMEM((chunks, own, tile), bf),
            dma((10,)), dma((8, 3)), dma((8, 3)), dma((8, 3)), dma((8, 3)),
            dma((3,)), dma((3,)), dma((3,)), dma((3,)), dma((3,)), dma((3,)), dma((1,)), dma((1,)),
            dma((3,)), dma((3,)), dma((4,)), dma((4,)),
            dma((chunks,)), dma((chunks,)), dma((chunks,)), dma((chunks,)), dma((chunks,)), dma((chunks,)),
            dma((chunks,)), dma((chunks,)),
        ],
        compiler_params=pltpu.CompilerParams(
            has_side_effects=True, collective_id=0, vmem_limit_bytes=60 * 2**20
        ),
    )(
        gate_weight, up_weight, dn, queries, forget_gate_logits, projected_values, output_gate_logits,
        extra_forget_logs, output_weight, residual,
        lower_bound_margin.reshape(1, channels), per_head_norm_gain.reshape(1, HD),
        feedforward_norm_gain.reshape(1, model),
    )


def fits(residual, queries, gate_weight):
    length, model = residual.shape
    share, half = gate_weight.shape
    return (
        lax.axis_size("sp") == 4 * GROUPS and lax.axis_size("tp") == 2 and share == HD
        and length % 256 == 0 and length <= 512 and half % (64 * GROUPS) == 0
        and queries.shape[1] == GROUPS * HD and model == 4 * GROUPS * share
    )


def local(
    residual,
    queries,
    forget_gate_logits,
    projected_values,
    output_gate_logits,
    lower_bound_margin,
    extra_forget_logs,
    per_head_norm_gain,
    output_weight,
    feedforward_norm_gain,
    gate_weight,
    up_weight,
    down_weight,
):
    if fits(residual, queries, gate_weight):
        return layer(
            residual, queries, forget_gate_logits, projected_values, output_gate_logits, lower_bound_margin,
            extra_forget_logs, per_head_norm_gain, output_weight, feedforward_norm_gain, gate_weight, up_weight, down_weight,
        )
    length = queries.shape[0]
    head_count = queries.shape[1] // HD
    state_increment = lower_bound_margin * jax.nn.sigmoid(-forget_gate_logits.astype(jnp.float32))
    retain_log_factor = jnp.log1p(-state_increment) + extra_forget_logs

    def to_blocks(source):
        return source.reshape(length // BLOCK, BLOCK, head_count, HD).transpose(0, 2, 1, 3)

    initial = (
        jnp.zeros((head_count, HD, HD), jnp.float32),
        jnp.zeros((head_count, HD), jnp.float32),
    )
    block_inputs = (
        to_blocks(queries.astype(jnp.float32)),
        to_blocks(state_increment),
        to_blocks(projected_values.astype(jnp.float32)),
        to_blocks(retain_log_factor),
    )
    (recurrent_state, decay_sum), (output_rows, rescaled_state) = lax.scan(
        block_update, initial, block_inputs
    )
    identity = (jnp.zeros_like(decay_sum), jnp.zeros_like(recurrent_state))
    incoming_state = carried_in_2((decay_sum, recurrent_state), "sp", join_states, identity)[1]
    output_rows = output_rows + jnp.einsum(
        "sjey,jyx->sjex", rescaled_state, incoming_state, precision=top_precision
    )
    mixed = output_rows.transpose(0, 2, 1, 3).reshape(length, head_count, HD)
    normed_heads = (
        mixed
        * lax.rsqrt(jnp.mean(mixed * mixed, axis=-1, keepdims=True) + eps)
        * per_head_norm_gain
    )
    gating = jax.nn.silu(output_gate_logits.astype(jnp.float32)).reshape(length, head_count, HD)
    gated = (normed_heads * gating).reshape(length, head_count * HD).astype(jnp.bfloat16)
    row_count = residual.shape[0] // lax.axis_size("tp")
    own_rows = lax.dynamic_slice_in_dim(residual, lax.axis_index("tp") * row_count, row_count, 0)
    rows_here = gated
    projected = lax.psum_scatter(
        jnp.dot(rows_here, output_weight, preferred_element_type=jnp.float32).astype(jnp.bfloat16),
        "tp",
        scatter_dimension=0,
        tiled=True,
    ).astype(jnp.float32)
    after_mixer = (own_rows.astype(jnp.float32) + projected).astype(jnp.bfloat16)
    widened = after_mixer.astype(jnp.float32)
    normed = (
        widened
        * lax.rsqrt(jnp.mean(widened * widened, axis=-1, keepdims=True) + eps)
        * feedforward_norm_gain
    ).astype(jnp.bfloat16)
    gate_full, up_full = (
        lax.all_gather(gate_weight, "sp", axis=0, tiled=True),
        lax.all_gather(up_weight, "sp", axis=0, tiled=True),
    )
    down_full = lax.all_gather(down_weight, "sp", axis=1, tiled=True)
    row_piece = lax.all_gather(normed, "tp", axis=0, tiled=True)
    gate_part = jnp.dot(row_piece, gate_full, preferred_element_type=jnp.float32)
    up_part = jnp.dot(row_piece, up_full, preferred_element_type=jnp.float32)
    hidden = (jax.nn.silu(gate_part) * up_part).astype(jnp.bfloat16)
    rows_here = hidden
    ffn_sum = lax.psum_scatter(
        jnp.dot(rows_here, down_full, preferred_element_type=jnp.float32).astype(jnp.bfloat16),
        "tp",
        scatter_dimension=0,
        tiled=True,
    ).astype(jnp.float32)
    finished = (after_mixer.astype(jnp.float32) + 0.5 * ffn_sum).astype(jnp.bfloat16)
    return lax.all_gather(finished, "tp", axis=0, tiled=True)


def solution(mesh):
    return jax.shard_map(
        local,
        mesh=mesh,
        in_specs=(
            P("sp", None),
            P("sp", "tp"),
            P("sp", "tp"),
            P("sp", "tp"),
            P("sp", "tp"),
            P("tp"),
            P("sp", "tp"),
            P(),
            P("tp", None),
            P(),
            P("sp", "tp"),
            P("sp", "tp"),
            P("tp", "sp"),
        ),
        out_specs=P("sp", None),
        check_vma=False,
    )
```

```python
import jax
import jax.numpy as jnp
from jax import lax
from jax.experimental import pallas as pl
from jax.experimental.pallas import tpu as pltpu
from jax.sharding import PartitionSpec as P

HD = 128
BLOCK = 64


eps = 1e-06
top_precision = lax.Precision.HIGHEST


def carried_in_2(value, axis, join, neutral):
    place = lax.axis_index(axis)
    gathered = jax.tree.map(
        lambda a, kind: lax.all_gather(a.astype(kind), axis), value, (jnp.bfloat16, jnp.bfloat16)
    )
    state = jax.tree.map(lambda a, e: jnp.zeros_like(a) + jnp.asarray(e, a.dtype), value, neutral)

    def one(turn, state):
        return join(
            state,
            jax.tree.map(
                lambda a, own: lax.dynamic_index_in_dim(a, turn, 0, False).astype(own.dtype),
                gathered,
                value,
            ),
        )

    return lax.fori_loop(0, place, one, state)


def block_update(carried_in, inputs):
    recurrent_state, offset = carried_in
    queries, state_increment, value_rows, retain_log_factor = inputs
    running_state = jnp.cumsum(retain_log_factor, axis=1)
    causal = jnp.tril(
        jnp.ones((retain_log_factor.shape[1], retain_log_factor.shape[1]), dtype=bool)
    )
    carried_over_state = jnp.einsum(
        "uqw,uwa->uqa", queries * jnp.exp(running_state), recurrent_state, precision=top_precision
    )
    spread = running_state[:, :, None, :] - running_state[:, None, :, :]
    weights = jnp.exp(jnp.where(causal[None, :, :, None], spread, -jnp.inf))
    scores = jnp.einsum(
        "htk,htsk,hsk->hts", queries, weights, state_increment, precision=top_precision
    )
    output_rows = carried_over_state + jnp.einsum(
        "hts,hsv->htv", scores, value_rows, precision=top_precision
    )
    final_state = running_state[:, -1:, :]
    updated_state = jnp.exp(final_state[:, 0, :])[:, :, None] * recurrent_state + jnp.einsum(
        "erb,erc->ebc",
        state_increment * jnp.exp(final_state - running_state),
        value_rows,
        precision=top_precision,
    )
    rescaled_state = queries * jnp.exp(running_state + offset[:, None, :])
    return ((updated_state, offset + final_state[:, 0, :]), (output_rows, rescaled_state))


def join_states(earlier, later):
    earlier_sum, earlier_memory = earlier
    later_sum, later_memory = later
    return (earlier_sum + later_sum, jnp.exp(later_sum)[:, :, None] * earlier_memory + later_memory)


MESH = pl.DeviceIdType.MESH
GROUPS = 4


def up_to(value, step):
    return -(-value // step) * step


def layer_kernel(
    dims, gate_hbm, up_hbm, dn_ref, q_hbm, f_hbm, v_hbm, og_hbm, extra_hbm, ow_hbm, res_hbm,
    margin_ref, head_gain_ref, ff_gain_ref, out_ref,
    gate_in, up_in, q_ref, f_ref, v_ref, og_ref, extra_ref, ow_ref, residual,
    gu_own, gu, dn, gu_pass, dn_pass, grown, q_grown, st_out, st_in, tot_out, tot_in, inc_out, inc,
    gated, proj, proj_got, x_own, rows_in, hid, part, peer_part, summed, xgot, pair, zgot,
    s_l, s_a, r_a, s_b, r_b, s_g, r_g, s_1, r_1, s_2, r_2, s_3, r_3, s_j, r_j, s_x, r_x, s_p, r_p,
    s_d, r_d, s_r, r_r, s_z, r_z, s_o, r_o,
):
    share, own, width, padded = dims
    me = lax.axis_index("sp")
    c = lax.axis_index("tp")
    z, r = me // 4, me % 4
    zh, zl, y, x = z // 2, z % 2, r // 2, r % 2
    inner = (zh + zl) % 2 == 1
    model = gu.shape[0]
    half = share // 2
    bf, f32 = jnp.bfloat16, jnp.float32

    def flip(value, d):
        return (value + d) % 2

    def place(o, dy=0):
        return (flip(zh, o // 4) * 2 + flip(zl, o // 2 % 2)) * 4 + flip(y, dy) * 2 + flip(x, o % 2)

    def group(o):
        return flip(x, o % 2) * 2 + flip(zl, o // 2 % 2)

    def beside(e):
        return flip(y, e // 2) * 2 + flip(x, e % 2)

    def remote(src, dst, send, recv, to, core):
        return pltpu.make_async_remote_copy(
            src_ref=src, dst_ref=dst, send_sem=send, recv_sem=recv, device_id=(to, core), device_id_type=MESH,
        )

    sent = []

    def go(copy):
        copy.start()
        sent.append(copy)
        return copy

    barrier = pltpu.get_barrier_semaphore()
    partners = [(place(o), c) for o in range(1, 8)] + [(place(0, 1), c), (place(1, 1), c), (me, 1 - c)]
    for partner in partners:
        pl.semaphore_signal(barrier, inc=1, device_id=partner, device_id_type=MESH)

    mine = pl.ds(pl.multiple_of(c * own, own), own)
    theirs = pl.ds(pl.multiple_of((1 - c) * own, own), own)
    loads = [
        pltpu.make_async_copy(src, dst, s_l.at[i])
        for i, (src, dst) in enumerate((
            (gate_hbm, gate_in), (up_hbm, up_in), (q_hbm, q_ref), (f_hbm, f_ref), (v_hbm, v_ref),
            (extra_hbm, extra_ref), (og_hbm, og_ref), (ow_hbm, ow_ref), (res_hbm.at[mine], residual),
            (dn_ref.at[group(0)], dn.at[pl.ds(0, width), pl.ds(pl.multiple_of(me * share, share), share)]),
        ))
    ]
    for load in loads:
        load.start()

    def region(owner, k):
        if k < 2:
            return gu.at[pl.ds(pl.multiple_of(owner * share + k * half, half), half)]
        return dn.at[pl.ds(0, width), pl.ds(pl.multiple_of(owner * share, share), share)]

    def origin(g, k):
        return gu_own.at[g, pl.ds(k * half, half)] if k < 2 else dn_ref.at[g]

    def passing(k):
        return gu_pass.at[pl.ds(k * half, half)] if k < 2 else dn_pass

    def direct(o, k):
        if o in (3, 5, 7):
            block = region(place(1), k)
            return remote(block if o == 5 else passing(k), block, s_a.at[o, k], r_a.at[o, k], place(o - 1), c)
        return remote(origin(group(o), k), region(me, k), s_a.at[o, k], r_a.at[o, k], place(o), c)

    passed = {}

    def pass_over(k):
        passed[k] = go(remote(origin(group(3), k), passing(k), s_g.at[k], r_g.at[k], place(1), c))

    def take(k):
        direct(1, k).wait_recv()

    def take_passed(k):
        copy = passed[k]
        copy.wait_recv()

    def lend(o, k):
        block = region(place(o), k)
        return remote(origin(group(0), k) if o == 0 else block, block, s_b.at[o, k], r_b.at[o, k], place(0, 1), c)

    def send(*pieces):
        for o, k in pieces:
            direct(o, k).start()

    def relay(*pieces):
        for o, k in pieces:
            if o > 1:
                direct(o, k).wait_recv()
            lend(o, k).start()

    def by_place(act, outer=(), between=()):
        @pl.when(inner)
        def _():
            act(*between)

        @pl.when(jnp.logical_not(inner))
        def _():
            act(*outer)

    if padded > width:
        dn[pl.ds(width, padded - width), :] = jnp.zeros((padded - width, model), dn.dtype)
    pl.semaphore_wait(barrier, len(partners))
    by_place(send, ((2, 2),), ((6, 2), (2, 2)))
    send((1, 2))
    relay((0, 2))
    loads[0].wait()
    loads[1].wait()
    even = width // 128 * 128
    for g in range(GROUPS):
        first = g * width
        gate, up = gate_in[:, first:first + width], up_in[:, first:first + width]
        for at in range(0, even, 128):
            gu_own[g, :, 2 * at:2 * at + 128] = gate[:, at:at + 128]
            gu_own[g, :, 2 * at + 128:2 * at + 256] = up[:, at:at + 128]
        if width > even:
            gu_own[g, :, 2 * even:] = jnp.concatenate([gate[:, even:], up[:, even:]], axis=1)
    gu[pl.ds(pl.multiple_of(me * share, share), share), :] = gu_own[group(0)]
    by_place(send, ((2, 0),), ((4, 0), (2, 0)))

    length, channels = q_ref.shape
    heads = channels // HD
    span = 128
    ones = lambda n: lax.broadcasted_iota(jnp.int32, (n, n), 0) >= lax.broadcasted_iota(jnp.int32, (n, n), 1)
    lower = ones(length).astype(f32)
    causal = ones(span)
    over = lambda p, q, i, j: lax.dot_general(p, q, (((i,), (j,)), ((), ())), preferred_element_type=f32)

    def logs_tile(logs):
        high = logs.astype(bf)
        low = (logs - high.astype(f32)).astype(bf)
        return jnp.concatenate([jnp.broadcast_to(high, (8, HD)), jnp.broadcast_to(low, (8, HD))], axis=0)

    def part_of(ref, at):
        tile = ref[at, HD:HD + 16, :].astype(f32)
        return tile[0:1] + tile[8:9], ref[at, 0:HD, :].astype(f32)

    for i in range(2, 6):
        loads[i].wait()
    for n in range(heads):
        cols = slice(n * HD, (n + 1) * HD)
        inflow = margin_ref[:, cols] * jax.nn.sigmoid(-f_ref[:, cols].astype(f32))
        keep = jnp.log1p(-inflow) + extra_ref[:, cols]
        total_log = lax.dot_general(lower, keep, (((1,), (0,)), ((), ())), precision=top_precision, preferred_element_type=f32)
        q = q_ref[:, cols].astype(f32)
        q_grown[:, cols] = (q * jnp.exp(total_log)).astype(bf)
        state = None
        for start in range(0, length, span):
            rows = slice(start, start + span)
            a, qb, ub, vb = total_log[rows], q[rows], inflow[rows], v_ref[rows, cols]
            middle, end = a[span // 2 - 1:span // 2], a[span - 1:span]
            scores = over((qb * jnp.exp(a - middle)).astype(bf), (ub * jnp.exp(middle - a)).astype(bf), 1, 1)
            mixed = over(jnp.where(causal, scores, 0.0).astype(bf), vb, 1, 0)
            added = over(vb, (ub * jnp.exp(end - a)).astype(bf), 0, 0)
            if state is None:
                state = added
            else:
                mixed = mixed + over((qb * jnp.exp(a - base)).astype(bf), state.astype(bf), 1, 1)
                state = state * jnp.exp(end - base) + added
            grown[rows, cols] = mixed
            base = end
        st_out[n, 0:HD, :] = state.astype(bf)
        st_out[n, HD:HD + 16, :] = logs_tile(base)

    to_head = [
        go(remote(st_out.at[beside(e)], st_in.at[r], s_1.at[e - 1], r_1.at[e - 1], z * 4 + beside(e), c)) for e in (3, 1, 2)
    ]
    st_in[r] = st_out[r]
    send((1, 0))
    pass_over(0)
    by_place(send, (), ((4, 1),))
    relay((0, 0), (0, 1))
    for copy in to_head:
        copy.wait_recv()
    whole, whole_log, before = jnp.zeros((HD, HD), f32), jnp.zeros((1, HD), f32), []
    for at in range(4):
        logs, state = part_of(st_in, at)
        before.append((whole_log, whole))
        whole = whole * jnp.exp(logs) + state
        whole_log = whole_log + logs
    tot_out[0, 0:HD, :] = whole.astype(bf)
    tot_out[0, HD:HD + 16, :] = logs_tile(whole_log)

    def total_to(d):
        return remote(tot_out.at[0], tot_in.at[z], s_2.at[d - 1], r_2.at[d - 1], place(2 * d), c)

    later = {1: zl == 0, 2: zh == 0, 3: zh == 0}
    for d in (2, 3, 1):
        @pl.when(later[d])
        def _():
            total_to(d).start()

    by_place(send, ((2, 1),), ((6, 0), (2, 1)))
    take(2)
    relay((1, 2))
    for d in (2, 3, 1):
        @pl.when(jnp.logical_not(later[d]))
        def _():
            total_to(d).wait_recv()

    state = jnp.zeros((HD, HD), f32)
    for at in range(3):
        logs, added = part_of(tot_in, at)
        state = jnp.where(at < z, state * jnp.exp(logs) + added, state)
    for at in range(4):
        early_log, early = before[at]
        inc_out[at] = (state * jnp.exp(early_log) + early).astype(bf)
    to_rows = [
        go(remote(inc_out.at[beside(e)], inc.at[r], s_3.at[e - 1], r_3.at[e - 1], z * 4 + beside(e), c)) for e in (3, 1, 2)
    ]
    inc[r] = inc_out[r]
    send((1, 1))
    pass_over(1)
    take(0)
    by_place(send, ((4, 0),), ((5, 0), (6, 1)))
    relay((1, 0))
    for i in range(6, 9):
        loads[i].wait()
    for copy in to_rows:
        copy.wait_recv()
    pass_over(2)
    take_passed(0)
    take(1)
    by_place(send, ((3, 0), (6, 0)), ((5, 1), (3, 0), (4, 2), (7, 0)))
    relay((2, 0), (2, 2))
    for n in range(heads):
        cols = slice(n * HD, (n + 1) * HD)
        mixed = grown[:, cols] + over(q_grown[:, cols], inc[n], 1, 1)
        scale = lax.rsqrt(jnp.mean(mixed * mixed, axis=-1, keepdims=True) + eps)
        gate = og_ref[:, cols].astype(f32)
        gated[:, cols] = (mixed * scale * head_gain_ref[...] * (gate * jax.nn.sigmoid(gate))).astype(bf)

    def project(rows):
        def step(j, carry):
            at = pl.multiple_of(j * 256, 256)
            proj[rows, pl.ds(at, 256)] = jnp.dot(
                gated[rows, :], ow_ref[:, pl.ds(at, 256)], preferred_element_type=f32
            ).astype(bf)
            return carry

        lax.fori_loop(0, model // 256, step, 0)

    project(theirs)
    joined = go(remote(proj.at[theirs], proj_got, s_j.at[0], r_j.at[0], me, 1 - c))
    project(mine)
    joined.wait_recv()
    after = (residual[...].astype(f32) + (proj[mine, :].astype(f32) + proj_got[...].astype(f32))).astype(bf)
    x_own[...] = after
    wide = after.astype(f32)
    normed = wide * lax.rsqrt(jnp.mean(wide * wide, axis=-1, keepdims=True) + eps) * ff_gain_ref[...]

    def token_rows(o):
        return pl.ds(pl.multiple_of((c * GROUPS + group(o)) * own, own), own)

    rows_in[token_rows(0), :] = normed.astype(bf)

    def rows_to(o, i, to, core):
        block = rows_in.at[token_rows(o)]
        return go(remote(block, block, s_x.at[i], r_x.at[i], to, core))

    def rows_over(o):
        block = rows_in.at[token_rows(o)]
        return go(remote(block, block, s_p.at[o], r_p.at[o], me, 1 - c))

    to_x, to_z = rows_to(0, 0, place(1), c), rows_to(0, 1, place(2), c)
    peers = [rows_over(0)]

    take_passed(1)
    by_place(send, (), ((7, 1),))
    relay((1, 1), (2, 1))
    by_place(relay, ((4, 0), (4, 1)), ((6, 0), (6, 1)))
    take_passed(2)
    by_place(send, (), ((7, 2),))
    to_z.wait_recv()
    to_x2 = rows_to(2, 2, place(1), c)
    peers.append(rows_over(2))
    by_place(
        send, ((7, 0), (4, 1), (6, 1), (5, 0), (7, 1), (5, 1), (3, 1), (3, 2), (4, 2), (6, 2), (5, 2), (7, 2)),
        ((3, 1), (3, 2), (5, 2)),
    )
    to_x.wait_recv()
    peers.append(rows_over(1))
    by_place(relay, ((5, 0), (6, 0)), ((4, 0), (7, 0), (3, 0)))
    to_x2.wait_recv()
    peers.append(rows_over(3))
    by_place(relay, ((5, 1), (3, 0)), ((7, 1), (6, 2)))
    by_place(relay, ((7, 0), (3, 1)), ((4, 1), (7, 2)))
    by_place(relay, ((6, 1), (7, 1)), ((5, 0), (5, 1), (3, 1)))
    by_place(relay, ((4, 2), (3, 2)), ())
    for copy in peers:
        copy.wait_recv()
    for o in range(8):
        for k in (0, 1):
            lend(o, k).wait_recv()

    block_rows = 4 * own

    def gate_up(m):
        rows = pl.ds(m * block_rows, block_rows)

        def step(j, carry):
            at = pl.multiple_of(j * 256, 256)
            both = jnp.dot(rows_in[rows, :], gu[:, pl.ds(at, 256)], preferred_element_type=f32)
            gate, up = both[:, :128], both[:, 128:]
            hid[rows, pl.ds(pl.multiple_of(j * 128, 128), 128)] = (gate * jax.nn.sigmoid(gate) * up).astype(bf)
            return carry

        lax.fori_loop(0, width // 128, step, 0)
        if width % 128:
            both = jnp.dot(rows_in[rows, :], gu[:, 2 * even:], preferred_element_type=f32)
            hid[rows, even:] = (both * jax.nn.sigmoid(both) * pltpu.roll(both, 64, 1)).astype(bf)

    gate_up(0)
    by_place(relay, ((5, 2),), ((3, 2),))
    gate_up(1)
    loads[9].wait()

    tile = 2 * share
    my_rows = pl.ds(pl.multiple_of(c * block_rows, block_rows), block_rows)
    their_rows = pl.ds(pl.multiple_of((1 - c) * block_rows, block_rows), block_rows)
    def group_rows(xx, zz):
        return pl.ds(pl.multiple_of((xx * 2 + zz) * own, own), own)

    def columns(k):
        at = (flip(zh, k // 4) * 2 + k // 2 % 2) * 4 + flip(y, k % 2) * 2
        return pl.ds(pl.multiple_of(at * share, tile), tile)

    def swap(k):
        return remote(part.at[k, their_rows], peer_part.at[k], s_d.at[k], r_d.at[k], me, 1 - c)

    def x_first(k):
        return k in (0, 1, 4, 5)

    def first_hop(k, i):
        if x_first(k):
            rows, to = group_rows(1 - x, i), place(1)
        else:
            rows, to = group_rows(i, 1 - zl), place(2)
        return remote(summed.at[k, rows], xgot.at[k, i], s_r.at[k, i], r_r.at[k, i], to, c)

    def second_hop(k):
        if x_first(k):
            return remote(pair.at[k, 1 - zl], zgot.at[k], s_z.at[k], r_z.at[k], place(2), c)
        return remote(pair.at[k, 1 - x], zgot.at[k], s_z.at[k], r_z.at[k], place(1), c)

    def finish(k):
        block = out_ref.at[mine, columns(k)]
        return remote(block, block, s_o.at[k], r_o.at[k], me, 1 - c)

    def down(k):
        for m in range(2):
            rows = pl.ds(m * block_rows, block_rows)
            part[k, rows, :] = jnp.dot(hid[rows, :], dn[:, columns(k)], preferred_element_type=f32).astype(bf)
        swap(k).start()

    def stage_1(k):
        swap(k).wait_recv()
        summed[k] = (part[k, my_rows, :].astype(f32) + peer_part[k].astype(f32)).astype(bf)
        for i in range(2):
            first_hop(k, i).start()

    def stage_2(k):
        for i in range(2):
            first_hop(k, i).wait_recv()
            rows = group_rows(x, i) if x_first(k) else group_rows(i, zl)
            pair[k, i] = (summed[k, rows, :].astype(f32) + xgot[k, i].astype(f32)).astype(bf)
        second_hop(k).start()

    def stage_3(k):
        second_hop(k).wait_recv()
        total = pair[k, zl if x_first(k) else x].astype(f32) + zgot[k].astype(f32)
        out_ref[mine, columns(k)] = (x_own[:, columns(k)].astype(f32) + 0.5 * total).astype(bf)
        finish(k).start()

    order = (0, 2, 1, 3, 4, 6, 5, 7)
    for turn in range(len(order) + 3):
        if turn == 0:
            by_place(relay, ((6, 2),), ((4, 2),))
        if turn == 1:
            by_place(relay, ((7, 2),), ((5, 2),))
        if turn == 2:
            for o in range(4):
                lend(o, 2).wait_recv()
        if turn == 6:
            for o in range(4, 8):
                lend(o, 2).wait_recv()
        if turn < len(order):
            down(order[turn])
        if 1 <= turn <= len(order):
            stage_1(order[turn - 1])
        if 2 <= turn <= len(order) + 1:
            stage_2(order[turn - 2])
        if turn >= 3:
            stage_3(order[turn - 3])
    for k in range(8):
        finish(k).wait_recv()
    for copy in sent:
        copy.wait_send()
    for d in (2, 3, 1):
        @pl.when(later[d])
        def _():
            total_to(d).wait_send()

    for o in range(8):
        for k in range(3):
            if o:
                direct(o, k).wait_send()
            lend(o, k).wait_send()
    for k in range(8):
        for copy in (swap(k), first_hop(k, 0), first_hop(k, 1), second_hop(k), finish(k)):
            copy.wait_send()


def layer(
    residual, queries, forget_gate_logits, projected_values, output_gate_logits, lower_bound_margin,
    extra_forget_logs, per_head_norm_gain, output_weight, feedforward_norm_gain, gate_weight, up_weight, down_weight,
):
    share, half = gate_weight.shape
    width = half // GROUPS
    padded = up_to(width, 128)
    length, model = residual.shape
    own = length // 2
    channels = queries.shape[1]
    dn = down_weight.reshape(GROUPS, width, share)
    bf, f32 = jnp.bfloat16, jnp.float32
    dma = pltpu.SemaphoreType.DMA
    dims = (share, own, width, padded)
    vm = pl.BlockSpec(memory_space=pltpu.VMEM)
    hbm = pl.BlockSpec(memory_space=pltpu.HBM)
    message = HD + 16
    tile = 2 * share
    chunks = model // tile
    return pl.pallas_call(
        lambda *refs: layer_kernel(dims, *refs),
        out_shape=jax.ShapeDtypeStruct((length, model), bf),
        in_specs=[hbm] * 10 + [vm] * 3,
        out_specs=vm,
        scratch_shapes=[
            pltpu.VMEM((share, half), bf),
            pltpu.VMEM((share, half), bf),
            pltpu.VMEM((length, channels), bf),
            pltpu.VMEM((length, channels), bf),
            pltpu.VMEM((length, channels), bf),
            pltpu.VMEM((length, channels), bf),
            pltpu.VMEM((length, channels), f32),
            pltpu.VMEM((channels, model), bf),
            pltpu.VMEM((own, model), bf),
            pltpu.VMEM((GROUPS, share, 2 * width), bf),
            pltpu.VMEM((model, 2 * width), bf),
            pltpu.VMEM((padded, model), bf),
            pltpu.VMEM((share, 2 * width), bf),
            pltpu.VMEM((width, share), bf),
            pltpu.VMEM((length, channels), f32),
            pltpu.VMEM((length, channels), bf),
            pltpu.VMEM((4, message, HD), bf),
            pltpu.VMEM((4, message, HD), bf),
            pltpu.VMEM((1, message, HD), bf),
            pltpu.VMEM((4, message, HD), bf),
            pltpu.VMEM((4, HD, HD), bf),
            pltpu.VMEM((4, HD, HD), bf),
            pltpu.VMEM((length, channels), bf),
            pltpu.VMEM((length, model), bf),
            pltpu.VMEM((own, model), bf),
            pltpu.VMEM((own, model), bf),
            pltpu.VMEM((GROUPS * length, model), bf),
            pltpu.VMEM((GROUPS * length, padded), bf),
            pltpu.VMEM((chunks, GROUPS * length, tile), bf),
            pltpu.VMEM((chunks, GROUPS * own, tile), bf),
            pltpu.VMEM((chunks, GROUPS * own, tile), bf),
            pltpu.VMEM((chunks, 2, own, tile), bf),
            pltpu.VMEM((chunks, 2, own, tile), bf),
            pltpu.VMEM((chunks, own, tile), bf),
            dma((10,)), dma((8, 3)), dma((8, 3)), dma((8, 3)), dma((8, 3)), dma((3,)), dma((3,)),
            dma((3,)), dma((3,)), dma((3,)), dma((3,)), dma((3,)), dma((3,)), dma((1,)), dma((1,)),
            dma((3,)), dma((3,)), dma((4,)), dma((4,)),
            dma((chunks,)), dma((chunks,)), dma((chunks, 2)), dma((chunks, 2)), dma((chunks,)), dma((chunks,)),
            dma((chunks,)), dma((chunks,)),
        ],
        compiler_params=pltpu.CompilerParams(
            has_side_effects=True, collective_id=0, vmem_limit_bytes=60 * 2**20
        ),
    )(
        gate_weight, up_weight, dn, queries, forget_gate_logits, projected_values, output_gate_logits,
        extra_forget_logs, output_weight, residual,
        lower_bound_margin.reshape(1, channels), per_head_norm_gain.reshape(1, HD),
        feedforward_norm_gain.reshape(1, model),
    )


def fits(residual, queries, gate_weight):
    length, model = residual.shape
    share, half = gate_weight.shape
    return (
        lax.axis_size("sp") == 4 * GROUPS and lax.axis_size("tp") == 2 and share == HD
        and length % 256 == 0 and length <= 512 and half % (64 * GROUPS) == 0
        and queries.shape[1] == GROUPS * HD and model == 4 * GROUPS * share
    )


def local(
    residual,
    queries,
    forget_gate_logits,
    projected_values,
    output_gate_logits,
    lower_bound_margin,
    extra_forget_logs,
    per_head_norm_gain,
    output_weight,
    feedforward_norm_gain,
    gate_weight,
    up_weight,
    down_weight,
):
    if fits(residual, queries, gate_weight):
        return layer(
            residual, queries, forget_gate_logits, projected_values, output_gate_logits, lower_bound_margin,
            extra_forget_logs, per_head_norm_gain, output_weight, feedforward_norm_gain, gate_weight, up_weight, down_weight,
        )
    length = queries.shape[0]
    head_count = queries.shape[1] // HD
    state_increment = lower_bound_margin * jax.nn.sigmoid(-forget_gate_logits.astype(jnp.float32))
    retain_log_factor = jnp.log1p(-state_increment) + extra_forget_logs

    def to_blocks(source):
        return source.reshape(length // BLOCK, BLOCK, head_count, HD).transpose(0, 2, 1, 3)

    initial = (
        jnp.zeros((head_count, HD, HD), jnp.float32),
        jnp.zeros((head_count, HD), jnp.float32),
    )
    block_inputs = (
        to_blocks(queries.astype(jnp.float32)),
        to_blocks(state_increment),
        to_blocks(projected_values.astype(jnp.float32)),
        to_blocks(retain_log_factor),
    )
    (recurrent_state, decay_sum), (output_rows, rescaled_state) = lax.scan(
        block_update, initial, block_inputs
    )
    identity = (jnp.zeros_like(decay_sum), jnp.zeros_like(recurrent_state))
    incoming_state = carried_in_2((decay_sum, recurrent_state), "sp", join_states, identity)[1]
    output_rows = output_rows + jnp.einsum(
        "sjey,jyx->sjex", rescaled_state, incoming_state, precision=top_precision
    )
    mixed = output_rows.transpose(0, 2, 1, 3).reshape(length, head_count, HD)
    normed_heads = (
        mixed
        * lax.rsqrt(jnp.mean(mixed * mixed, axis=-1, keepdims=True) + eps)
        * per_head_norm_gain
    )
    gating = jax.nn.silu(output_gate_logits.astype(jnp.float32)).reshape(length, head_count, HD)
    gated = (normed_heads * gating).reshape(length, head_count * HD).astype(jnp.bfloat16)
    row_count = residual.shape[0] // lax.axis_size("tp")
    own_rows = lax.dynamic_slice_in_dim(residual, lax.axis_index("tp") * row_count, row_count, 0)
    rows_here = gated
    projected = lax.psum_scatter(
        jnp.dot(rows_here, output_weight, preferred_element_type=jnp.float32).astype(jnp.bfloat16),
        "tp",
        scatter_dimension=0,
        tiled=True,
    ).astype(jnp.float32)
    after_mixer = (own_rows.astype(jnp.float32) + projected).astype(jnp.bfloat16)
    widened = after_mixer.astype(jnp.float32)
    normed = (
        widened
        * lax.rsqrt(jnp.mean(widened * widened, axis=-1, keepdims=True) + eps)
        * feedforward_norm_gain
    ).astype(jnp.bfloat16)
    gate_full, up_full = (
        lax.all_gather(gate_weight, "sp", axis=0, tiled=True),
        lax.all_gather(up_weight, "sp", axis=0, tiled=True),
    )
    down_full = lax.all_gather(down_weight, "sp", axis=1, tiled=True)
    row_piece = lax.all_gather(normed, "tp", axis=0, tiled=True)
    gate_part = jnp.dot(row_piece, gate_full, preferred_element_type=jnp.float32)
    up_part = jnp.dot(row_piece, up_full, preferred_element_type=jnp.float32)
    hidden = (jax.nn.silu(gate_part) * up_part).astype(jnp.bfloat16)
    rows_here = hidden
    ffn_sum = lax.psum_scatter(
        jnp.dot(rows_here, down_full, preferred_element_type=jnp.float32).astype(jnp.bfloat16),
        "tp",
        scatter_dimension=0,
        tiled=True,
    ).astype(jnp.float32)
    finished = (after_mixer.astype(jnp.float32) + 0.5 * ffn_sum).astype(jnp.bfloat16)
    return lax.all_gather(finished, "tp", axis=0, tiled=True)


def solution(mesh):
    return jax.shard_map(
        local,
        mesh=mesh,
        in_specs=(
            P("sp", None),
            P("sp", "tp"),
            P("sp", "tp"),
            P("sp", "tp"),
            P("sp", "tp"),
            P("tp"),
            P("sp", "tp"),
            P(),
            P("tp", None),
            P(),
            P("sp", "tp"),
            P("sp", "tp"),
            P("tp", "sp"),
        ),
        out_specs=P("sp", None),
        check_vma=False,
    )
```

```python
import jax
import jax.numpy as jnp
from jax import lax
from jax.experimental import pallas as pl
from jax.experimental.pallas import tpu as pltpu
from jax.sharding import PartitionSpec as P

HD = 128
BLOCK = 64


eps = 1e-06
top_precision = lax.Precision.HIGHEST


def carried_in_2(value, axis, join, neutral):
    place = lax.axis_index(axis)
    gathered = jax.tree.map(
        lambda a, kind: lax.all_gather(a.astype(kind), axis), value, (jnp.bfloat16, jnp.bfloat16)
    )
    state = jax.tree.map(lambda a, e: jnp.zeros_like(a) + jnp.asarray(e, a.dtype), value, neutral)

    def one(turn, state):
        return join(
            state,
            jax.tree.map(
                lambda a, own: lax.dynamic_index_in_dim(a, turn, 0, False).astype(own.dtype),
                gathered,
                value,
            ),
        )

    return lax.fori_loop(0, place, one, state)


def block_update(carried_in, inputs):
    recurrent_state, offset = carried_in
    queries, state_increment, value_rows, retain_log_factor = inputs
    running_state = jnp.cumsum(retain_log_factor, axis=1)
    causal = jnp.tril(
        jnp.ones((retain_log_factor.shape[1], retain_log_factor.shape[1]), dtype=bool)
    )
    carried_over_state = jnp.einsum(
        "uqw,uwa->uqa", queries * jnp.exp(running_state), recurrent_state, precision=top_precision
    )
    spread = running_state[:, :, None, :] - running_state[:, None, :, :]
    weights = jnp.exp(jnp.where(causal[None, :, :, None], spread, -jnp.inf))
    scores = jnp.einsum(
        "htk,htsk,hsk->hts", queries, weights, state_increment, precision=top_precision
    )
    output_rows = carried_over_state + jnp.einsum(
        "hts,hsv->htv", scores, value_rows, precision=top_precision
    )
    final_state = running_state[:, -1:, :]
    updated_state = jnp.exp(final_state[:, 0, :])[:, :, None] * recurrent_state + jnp.einsum(
        "erb,erc->ebc",
        state_increment * jnp.exp(final_state - running_state),
        value_rows,
        precision=top_precision,
    )
    rescaled_state = queries * jnp.exp(running_state + offset[:, None, :])
    return ((updated_state, offset + final_state[:, 0, :]), (output_rows, rescaled_state))


def join_states(earlier, later):
    earlier_sum, earlier_memory = earlier
    later_sum, later_memory = later
    return (earlier_sum + later_sum, jnp.exp(later_sum)[:, :, None] * earlier_memory + later_memory)


MESH = pl.DeviceIdType.MESH
GROUPS = 4


def up_to(value, step):
    return -(-value // step) * step


def layer_kernel(
    dims, gate_hbm, up_hbm, dn_ref, q_hbm, f_hbm, v_hbm, og_hbm, extra_hbm, ow_hbm, res_hbm,
    margin_ref, head_gain_ref, ff_gain_ref, out_ref,
    gate_in, up_in, q_ref, f_ref, v_ref, og_ref, extra_ref, ow_ref, residual,
    gu_own, gu, dn, gu_pass, dn_pass, grown, q_grown, st_out, st_in, tot_out, tot_in, inc_out, inc,
    gated, proj, proj_got, x_own, rows_in, hid, part, peer_part, summed, xgot, pair, zgot,
    s_l, s_a, r_a, s_b, r_b, s_g, r_g, s_1, r_1, s_2, r_2, s_3, r_3, s_j, r_j, s_x, r_x, s_p, r_p,
    s_d, r_d, s_r, r_r, s_z, r_z, s_o, r_o,
):
    share, own, width, padded = dims
    me = lax.axis_index("sp")
    c = lax.axis_index("tp")
    z, r = me // 4, me % 4
    zh, zl, y, x = z // 2, z % 2, r // 2, r % 2
    inner = (zh + zl) % 2 == 1
    model = gu.shape[0]
    half = share // 2
    bf, f32 = jnp.bfloat16, jnp.float32

    def flip(value, d):
        return (value + d) % 2

    def place(o, dy=0):
        return (flip(zh, o // 4) * 2 + flip(zl, o // 2 % 2)) * 4 + flip(y, dy) * 2 + flip(x, o % 2)

    def group(o):
        return flip(x, o % 2) * 2 + flip(zl, o // 2 % 2)

    def beside(e):
        return flip(y, e // 2) * 2 + flip(x, e % 2)

    def remote(src, dst, send, recv, to, core):
        return pltpu.make_async_remote_copy(
            src_ref=src, dst_ref=dst, send_sem=send, recv_sem=recv, device_id=(to, core), device_id_type=MESH,
        )

    sent = []

    def go(copy):
        copy.start()
        sent.append(copy)
        return copy

    barrier = pltpu.get_barrier_semaphore()
    partners = [(place(o), c) for o in range(1, 8)] + [(place(0, 1), c), (place(1, 1), c), (me, 1 - c)]
    for partner in partners:
        pl.semaphore_signal(barrier, inc=1, device_id=partner, device_id_type=MESH)

    mine = pl.ds(pl.multiple_of(c * own, own), own)
    theirs = pl.ds(pl.multiple_of((1 - c) * own, own), own)
    loads = [
        pltpu.make_async_copy(src, dst, s_l.at[i])
        for i, (src, dst) in enumerate((
            (gate_hbm, gate_in), (up_hbm, up_in), (q_hbm, q_ref), (f_hbm, f_ref), (v_hbm, v_ref),
            (extra_hbm, extra_ref), (og_hbm, og_ref), (ow_hbm, ow_ref), (res_hbm.at[mine], residual),
            (dn_ref.at[group(0)], dn.at[pl.ds(0, width), pl.ds(pl.multiple_of(me * share, share), share)]),
        ))
    ]
    for load in loads:
        load.start()

    def region(owner, k):
        if k < 2:
            return gu.at[pl.ds(pl.multiple_of(owner * share + k * half, half), half)]
        return dn.at[pl.ds(0, width), pl.ds(pl.multiple_of(owner * share, share), share)]

    def origin(g, k):
        return gu_own.at[g, pl.ds(k * half, half)] if k < 2 else dn_ref.at[g]

    def passing(k):
        return gu_pass.at[pl.ds(k * half, half)] if k < 2 else dn_pass

    def direct(o, k):
        if o in (3, 5, 7):
            block = region(place(1), k)
            return remote(block if o == 5 else passing(k), block, s_a.at[o, k], r_a.at[o, k], place(o - 1), c)
        return remote(origin(group(o), k), region(me, k), s_a.at[o, k], r_a.at[o, k], place(o), c)

    passed = {}

    def pass_over(k):
        passed[k] = go(remote(origin(group(3), k), passing(k), s_g.at[k], r_g.at[k], place(1), c))

    def take(k):
        direct(1, k).wait_recv()

    def take_passed(k):
        copy = passed[k]
        copy.wait_recv()

    def lend(o, k):
        block = region(place(o), k)
        return remote(origin(group(0), k) if o == 0 else block, block, s_b.at[o, k], r_b.at[o, k], place(0, 1), c)

    def send(*pieces):
        for o, k in pieces:
            direct(o, k).start()

    def relay(*pieces):
        for o, k in pieces:
            if o > 1:
                direct(o, k).wait_recv()
            lend(o, k).start()

    def by_place(act, outer=(), between=()):
        @pl.when(inner)
        def _():
            act(*between)

        @pl.when(jnp.logical_not(inner))
        def _():
            act(*outer)

    if padded > width:
        dn[pl.ds(width, padded - width), :] = jnp.zeros((padded - width, model), dn.dtype)
    pl.semaphore_wait(barrier, len(partners))
    by_place(send, ((2, 2),), ((4, 2),))
    send((1, 2))
    relay((0, 2))
    loads[0].wait()
    loads[1].wait()
    even = width // 128 * 128
    for g in range(GROUPS):
        first = g * width
        gate, up = gate_in[:, first:first + width], up_in[:, first:first + width]
        for at in range(0, even, 128):
            gu_own[g, :, 2 * at:2 * at + 128] = gate[:, at:at + 128]
            gu_own[g, :, 2 * at + 128:2 * at + 256] = up[:, at:at + 128]
        if width > even:
            gu_own[g, :, 2 * even:] = jnp.concatenate([gate[:, even:], up[:, even:]], axis=1)
    gu[pl.ds(pl.multiple_of(me * share, share), share), :] = gu_own[group(0)]
    by_place(send, ((2, 0),), ((4, 0), (2, 0)))

    length, channels = q_ref.shape
    heads = channels // HD
    span = 128
    ones = lambda n: lax.broadcasted_iota(jnp.int32, (n, n), 0) >= lax.broadcasted_iota(jnp.int32, (n, n), 1)
    lower = ones(length).astype(f32)
    causal = ones(span)
    over = lambda p, q, i, j: lax.dot_general(p, q, (((i,), (j,)), ((), ())), preferred_element_type=f32)

    def logs_tile(logs):
        high = logs.astype(bf)
        low = (logs - high.astype(f32)).astype(bf)
        return jnp.concatenate([jnp.broadcast_to(high, (8, HD)), jnp.broadcast_to(low, (8, HD))], axis=0)

    def part_of(ref, at):
        tile = ref[at, HD:HD + 16, :].astype(f32)
        return tile[0:1] + tile[8:9], ref[at, 0:HD, :].astype(f32)

    for i in range(2, 6):
        loads[i].wait()
    for n in range(heads):
        cols = slice(n * HD, (n + 1) * HD)
        inflow = margin_ref[:, cols] * jax.nn.sigmoid(-f_ref[:, cols].astype(f32))
        keep = jnp.log1p(-inflow) + extra_ref[:, cols]
        total_log = lax.dot_general(lower, keep, (((1,), (0,)), ((), ())), precision=top_precision, preferred_element_type=f32)
        q = q_ref[:, cols].astype(f32)
        q_grown[:, cols] = (q * jnp.exp(total_log)).astype(bf)
        state = None
        for start in range(0, length, span):
            rows = slice(start, start + span)
            a, qb, ub, vb = total_log[rows], q[rows], inflow[rows], v_ref[rows, cols]
            middle, end = a[span // 2 - 1:span // 2], a[span - 1:span]
            scores = over((qb * jnp.exp(a - middle)).astype(bf), (ub * jnp.exp(middle - a)).astype(bf), 1, 1)
            mixed = over(jnp.where(causal, scores, 0.0).astype(bf), vb, 1, 0)
            added = over(vb, (ub * jnp.exp(end - a)).astype(bf), 0, 0)
            if state is None:
                state = added
            else:
                mixed = mixed + over((qb * jnp.exp(a - base)).astype(bf), state.astype(bf), 1, 1)
                state = state * jnp.exp(end - base) + added
            grown[rows, cols] = mixed
            base = end
        st_out[n, 0:HD, :] = state.astype(bf)
        st_out[n, HD:HD + 16, :] = logs_tile(base)

    to_head = [
        go(remote(st_out.at[beside(e)], st_in.at[r], s_1.at[e - 1], r_1.at[e - 1], z * 4 + beside(e), c)) for e in (3, 1, 2)
    ]
    st_in[r] = st_out[r]
    send((1, 0))
    pass_over(0)
    by_place(send, (), ((4, 1),))
    relay((0, 0), (0, 1))
    for copy in to_head:
        copy.wait_recv()
    whole, whole_log, before = jnp.zeros((HD, HD), f32), jnp.zeros((1, HD), f32), []
    for at in range(4):
        logs, state = part_of(st_in, at)
        before.append((whole_log, whole))
        whole = whole * jnp.exp(logs) + state
        whole_log = whole_log + logs
    tot_out[0, 0:HD, :] = whole.astype(bf)
    tot_out[0, HD:HD + 16, :] = logs_tile(whole_log)

    def total_to(d):
        return remote(tot_out.at[0], tot_in.at[z], s_2.at[d - 1], r_2.at[d - 1], place(2 * d), c)

    later = {1: zl == 0, 2: zh == 0, 3: zh == 0}
    for d in (2, 3, 1):
        @pl.when(later[d])
        def _():
            total_to(d).start()

    by_place(send, ((2, 1),), ((6, 0), (2, 1), (2, 2)))
    take(2)
    relay((1, 2))
    for d in (2, 3, 1):
        @pl.when(jnp.logical_not(later[d]))
        def _():
            total_to(d).wait_recv()

    state = jnp.zeros((HD, HD), f32)
    for at in range(3):
        logs, added = part_of(tot_in, at)
        state = jnp.where(at < z, state * jnp.exp(logs) + added, state)
    for at in range(4):
        early_log, early = before[at]
        inc_out[at] = (state * jnp.exp(early_log) + early).astype(bf)
    to_rows = [
        go(remote(inc_out.at[beside(e)], inc.at[r], s_3.at[e - 1], r_3.at[e - 1], z * 4 + beside(e), c)) for e in (3, 1, 2)
    ]
    inc[r] = inc_out[r]
    send((1, 1))
    pass_over(1)
    take(0)
    by_place(send, ((4, 0),), ((5, 0), (6, 1)))
    relay((1, 0))
    for i in range(6, 9):
        loads[i].wait()
    for copy in to_rows:
        copy.wait_recv()
    pass_over(2)
    take_passed(0)
    take(1)
    by_place(send, ((3, 0),), ((5, 1), (3, 0), (7, 0)))
    by_place(relay, ((2, 0),), ((2, 0), (2, 2)))
    for n in range(heads):
        cols = slice(n * HD, (n + 1) * HD)
        mixed = grown[:, cols] + over(q_grown[:, cols], inc[n], 1, 1)
        scale = lax.rsqrt(jnp.mean(mixed * mixed, axis=-1, keepdims=True) + eps)
        gate = og_ref[:, cols].astype(f32)
        gated[:, cols] = (mixed * scale * head_gain_ref[...] * (gate * jax.nn.sigmoid(gate))).astype(bf)

    def project(rows):
        def step(j, carry):
            at = pl.multiple_of(j * 256, 256)
            proj[rows, pl.ds(at, 256)] = jnp.dot(
                gated[rows, :], ow_ref[:, pl.ds(at, 256)], preferred_element_type=f32
            ).astype(bf)
            return carry

        lax.fori_loop(0, model // 256, step, 0)

    project(theirs)
    joined = go(remote(proj.at[theirs], proj_got, s_j.at[0], r_j.at[0], me, 1 - c))
    project(mine)
    joined.wait_recv()
    after = (residual[...].astype(f32) + (proj[mine, :].astype(f32) + proj_got[...].astype(f32))).astype(bf)
    x_own[...] = after
    wide = after.astype(f32)
    normed = wide * lax.rsqrt(jnp.mean(wide * wide, axis=-1, keepdims=True) + eps) * ff_gain_ref[...]

    def token_rows(o):
        return pl.ds(pl.multiple_of((c * GROUPS + group(o)) * own, own), own)

    rows_in[token_rows(0), :] = normed.astype(bf)

    def rows_to(o, i, to, core):
        block = rows_in.at[token_rows(o)]
        return go(remote(block, block, s_x.at[i], r_x.at[i], to, core))

    def rows_over(o):
        block = rows_in.at[token_rows(o)]
        return go(remote(block, block, s_p.at[o], r_p.at[o], me, 1 - c))

    to_x, to_z = rows_to(0, 0, place(1), c), rows_to(0, 1, place(2), c)
    peers = [rows_over(0)]

    take_passed(1)
    take_passed(2)
    by_place(
        send, ((3, 1), (4, 1), (5, 0), (5, 1), (7, 0), (6, 0), (6, 1), (7, 1), (6, 2), (3, 2), (7, 2), (4, 2), (5, 2)),
        ((7, 1), (7, 2), (6, 2)),
    )
    relay((1, 1), (2, 1))
    by_place(relay, ((4, 0), (4, 1), (2, 2)), ((6, 0), (6, 1)))
    to_z.wait_recv()
    to_x2 = rows_to(2, 2, place(1), c)
    peers.append(rows_over(2))
    by_place(send, (), ((3, 1), (3, 2), (5, 2)))
    to_x.wait_recv()
    peers.append(rows_over(1))
    by_place(relay, ((4, 2), (5, 0)), ((4, 0), (7, 0), (3, 0)))
    to_x2.wait_recv()
    peers.append(rows_over(3))
    by_place(relay, ((5, 1), (3, 0)), ((3, 1), (4, 1)))
    by_place(relay, ((3, 1), (7, 0)), ((7, 1), (5, 0)))
    by_place(relay, ((6, 0), (6, 1), (7, 1)), ((5, 1),))
    by_place(relay, ((3, 2),), ())
    for copy in peers:
        copy.wait_recv()
    for o in range(8):
        for k in (0, 1):
            lend(o, k).wait_recv()

    block_rows = 4 * own

    def gate_up(m):
        rows = pl.ds(m * block_rows, block_rows)

        def step(j, carry):
            at = pl.multiple_of(j * 256, 256)
            both = jnp.dot(rows_in[rows, :], gu[:, pl.ds(at, 256)], preferred_element_type=f32)
            gate, up = both[:, :128], both[:, 128:]
            hid[rows, pl.ds(pl.multiple_of(j * 128, 128), 128)] = (gate * jax.nn.sigmoid(gate) * up).astype(bf)
            return carry

        lax.fori_loop(0, width // 128, step, 0)
        if width % 128:
            both = jnp.dot(rows_in[rows, :], gu[:, 2 * even:], preferred_element_type=f32)
            hid[rows, even:] = (both * jax.nn.sigmoid(both) * pltpu.roll(both, 64, 1)).astype(bf)

    gate_up(0)
    by_place(relay, ((6, 2),), ((3, 2),))
    gate_up(1)
    loads[9].wait()

    tile = 2 * share
    my_rows = pl.ds(pl.multiple_of(c * block_rows, block_rows), block_rows)
    their_rows = pl.ds(pl.multiple_of((1 - c) * block_rows, block_rows), block_rows)
    def group_rows(xx, zz):
        return pl.ds(pl.multiple_of((xx * 2 + zz) * own, own), own)

    def columns(k):
        at = (flip(zh, k // 4) * 2 + k // 2 % 2) * 4 + flip(y, k % 2) * 2
        return pl.ds(pl.multiple_of(at * share, tile), tile)

    def swap(k):
        return remote(part.at[k, their_rows], peer_part.at[k], s_d.at[k], r_d.at[k], me, 1 - c)

    def x_first(k):
        return k in (0, 1, 4, 5)

    def first_hop(k, i):
        if x_first(k):
            rows, to = group_rows(1 - x, i), place(1)
        else:
            rows, to = group_rows(i, 1 - zl), place(2)
        return remote(summed.at[k, rows], xgot.at[k, i], s_r.at[k, i], r_r.at[k, i], to, c)

    def second_hop(k):
        if x_first(k):
            return remote(pair.at[k, 1 - zl], zgot.at[k], s_z.at[k], r_z.at[k], place(2), c)
        return remote(pair.at[k, 1 - x], zgot.at[k], s_z.at[k], r_z.at[k], place(1), c)

    def finish(k):
        block = out_ref.at[mine, columns(k)]
        return remote(block, block, s_o.at[k], r_o.at[k], me, 1 - c)

    def down(k):
        for m in range(2):
            rows = pl.ds(m * block_rows, block_rows)
            part[k, rows, :] = jnp.dot(hid[rows, :], dn[:, columns(k)], preferred_element_type=f32).astype(bf)
        swap(k).start()

    def stage_1(k):
        swap(k).wait_recv()
        summed[k] = (part[k, my_rows, :].astype(f32) + peer_part[k].astype(f32)).astype(bf)
        for i in range(2):
            first_hop(k, i).start()

    def stage_2(k):
        for i in range(2):
            first_hop(k, i).wait_recv()
            rows = group_rows(x, i) if x_first(k) else group_rows(i, zl)
            pair[k, i] = (summed[k, rows, :].astype(f32) + xgot[k, i].astype(f32)).astype(bf)
        second_hop(k).start()

    def stage_3(k):
        second_hop(k).wait_recv()
        total = pair[k, zl if x_first(k) else x].astype(f32) + zgot[k].astype(f32)
        out_ref[mine, columns(k)] = (x_own[:, columns(k)].astype(f32) + 0.5 * total).astype(bf)
        finish(k).start()

    order = (0, 2, 1, 3, 4, 6, 5, 7)
    for turn in range(len(order) + 3):
        if turn == 0:
            by_place(relay, ((7, 2),), ((4, 2),))
        if turn == 1:
            by_place(relay, ((5, 2),), ((5, 2), (7, 2), (6, 2)))
        if turn == 2:
            for o in range(4):
                lend(o, 2).wait_recv()
        if turn == 6:
            for o in range(4, 8):
                lend(o, 2).wait_recv()
        if turn < len(order):
            down(order[turn])
        if 1 <= turn <= len(order):
            stage_1(order[turn - 1])
        if 2 <= turn <= len(order) + 1:
            stage_2(order[turn - 2])
        if turn >= 3:
            stage_3(order[turn - 3])
    for k in range(8):
        finish(k).wait_recv()
    for copy in sent:
        copy.wait_send()
    for d in (2, 3, 1):
        @pl.when(later[d])
        def _():
            total_to(d).wait_send()

    for o in range(8):
        for k in range(3):
            if o:
                direct(o, k).wait_send()
            lend(o, k).wait_send()
    for k in range(8):
        for copy in (swap(k), first_hop(k, 0), first_hop(k, 1), second_hop(k), finish(k)):
            copy.wait_send()


def layer(
    residual, queries, forget_gate_logits, projected_values, output_gate_logits, lower_bound_margin,
    extra_forget_logs, per_head_norm_gain, output_weight, feedforward_norm_gain, gate_weight, up_weight, down_weight,
):
    share, half = gate_weight.shape
    width = half // GROUPS
    padded = up_to(width, 128)
    length, model = residual.shape
    own = length // 2
    channels = queries.shape[1]
    dn = down_weight.reshape(GROUPS, width, share)
    bf, f32 = jnp.bfloat16, jnp.float32
    dma = pltpu.SemaphoreType.DMA
    dims = (share, own, width, padded)
    vm = pl.BlockSpec(memory_space=pltpu.VMEM)
    hbm = pl.BlockSpec(memory_space=pltpu.HBM)
    message = HD + 16
    tile = 2 * share
    chunks = model // tile
    return pl.pallas_call(
        lambda *refs: layer_kernel(dims, *refs),
        out_shape=jax.ShapeDtypeStruct((length, model), bf),
        in_specs=[hbm] * 10 + [vm] * 3,
        out_specs=vm,
        scratch_shapes=[
            pltpu.VMEM((share, half), bf),
            pltpu.VMEM((share, half), bf),
            pltpu.VMEM((length, channels), bf),
            pltpu.VMEM((length, channels), bf),
            pltpu.VMEM((length, channels), bf),
            pltpu.VMEM((length, channels), bf),
            pltpu.VMEM((length, channels), f32),
            pltpu.VMEM((channels, model), bf),
            pltpu.VMEM((own, model), bf),
            pltpu.VMEM((GROUPS, share, 2 * width), bf),
            pltpu.VMEM((model, 2 * width), bf),
            pltpu.VMEM((padded, model), bf),
            pltpu.VMEM((share, 2 * width), bf),
            pltpu.VMEM((width, share), bf),
            pltpu.VMEM((length, channels), f32),
            pltpu.VMEM((length, channels), bf),
            pltpu.VMEM((4, message, HD), bf),
            pltpu.VMEM((4, message, HD), bf),
            pltpu.VMEM((1, message, HD), bf),
            pltpu.VMEM((4, message, HD), bf),
            pltpu.VMEM((4, HD, HD), bf),
            pltpu.VMEM((4, HD, HD), bf),
            pltpu.VMEM((length, channels), bf),
            pltpu.VMEM((length, model), bf),
            pltpu.VMEM((own, model), bf),
            pltpu.VMEM((own, model), bf),
            pltpu.VMEM((GROUPS * length, model), bf),
            pltpu.VMEM((GROUPS * length, padded), bf),
            pltpu.VMEM((chunks, GROUPS * length, tile), bf),
            pltpu.VMEM((chunks, GROUPS * own, tile), bf),
            pltpu.VMEM((chunks, GROUPS * own, tile), bf),
            pltpu.VMEM((chunks, 2, own, tile), bf),
            pltpu.VMEM((chunks, 2, own, tile), bf),
            pltpu.VMEM((chunks, own, tile), bf),
            dma((10,)), dma((8, 3)), dma((8, 3)), dma((8, 3)), dma((8, 3)), dma((3,)), dma((3,)),
            dma((3,)), dma((3,)), dma((3,)), dma((3,)), dma((3,)), dma((3,)), dma((1,)), dma((1,)),
            dma((3,)), dma((3,)), dma((4,)), dma((4,)),
            dma((chunks,)), dma((chunks,)), dma((chunks, 2)), dma((chunks, 2)), dma((chunks,)), dma((chunks,)),
            dma((chunks,)), dma((chunks,)),
        ],
        compiler_params=pltpu.CompilerParams(
            has_side_effects=True, collective_id=0, vmem_limit_bytes=60 * 2**20
        ),
    )(
        gate_weight, up_weight, dn, queries, forget_gate_logits, projected_values, output_gate_logits,
        extra_forget_logs, output_weight, residual,
        lower_bound_margin.reshape(1, channels), per_head_norm_gain.reshape(1, HD),
        feedforward_norm_gain.reshape(1, model),
    )


def fits(residual, queries, gate_weight):
    length, model = residual.shape
    share, half = gate_weight.shape
    return (
        lax.axis_size("sp") == 4 * GROUPS and lax.axis_size("tp") == 2 and share == HD
        and length % 256 == 0 and length <= 512 and half % (64 * GROUPS) == 0
        and queries.shape[1] == GROUPS * HD and model == 4 * GROUPS * share
    )


def local(
    residual,
    queries,
    forget_gate_logits,
    projected_values,
    output_gate_logits,
    lower_bound_margin,
    extra_forget_logs,
    per_head_norm_gain,
    output_weight,
    feedforward_norm_gain,
    gate_weight,
    up_weight,
    down_weight,
):
    if fits(residual, queries, gate_weight):
        return layer(
            residual, queries, forget_gate_logits, projected_values, output_gate_logits, lower_bound_margin,
            extra_forget_logs, per_head_norm_gain, output_weight, feedforward_norm_gain, gate_weight, up_weight, down_weight,
        )
    length = queries.shape[0]
    head_count = queries.shape[1] // HD
    state_increment = lower_bound_margin * jax.nn.sigmoid(-forget_gate_logits.astype(jnp.float32))
    retain_log_factor = jnp.log1p(-state_increment) + extra_forget_logs

    def to_blocks(source):
        return source.reshape(length // BLOCK, BLOCK, head_count, HD).transpose(0, 2, 1, 3)

    initial = (
        jnp.zeros((head_count, HD, HD), jnp.float32),
        jnp.zeros((head_count, HD), jnp.float32),
    )
    block_inputs = (
        to_blocks(queries.astype(jnp.float32)),
        to_blocks(state_increment),
        to_blocks(projected_values.astype(jnp.float32)),
        to_blocks(retain_log_factor),
    )
    (recurrent_state, decay_sum), (output_rows, rescaled_state) = lax.scan(
        block_update, initial, block_inputs
    )
    identity = (jnp.zeros_like(decay_sum), jnp.zeros_like(recurrent_state))
    incoming_state = carried_in_2((decay_sum, recurrent_state), "sp", join_states, identity)[1]
    output_rows = output_rows + jnp.einsum(
        "sjey,jyx->sjex", rescaled_state, incoming_state, precision=top_precision
    )
    mixed = output_rows.transpose(0, 2, 1, 3).reshape(length, head_count, HD)
    normed_heads = (
        mixed
        * lax.rsqrt(jnp.mean(mixed * mixed, axis=-1, keepdims=True) + eps)
        * per_head_norm_gain
    )
    gating = jax.nn.silu(output_gate_logits.astype(jnp.float32)).reshape(length, head_count, HD)
    gated = (normed_heads * gating).reshape(length, head_count * HD).astype(jnp.bfloat16)
    row_count = residual.shape[0] // lax.axis_size("tp")
    own_rows = lax.dynamic_slice_in_dim(residual, lax.axis_index("tp") * row_count, row_count, 0)
    rows_here = gated
    projected = lax.psum_scatter(
        jnp.dot(rows_here, output_weight, preferred_element_type=jnp.float32).astype(jnp.bfloat16),
        "tp",
        scatter_dimension=0,
        tiled=True,
    ).astype(jnp.float32)
    after_mixer = (own_rows.astype(jnp.float32) + projected).astype(jnp.bfloat16)
    widened = after_mixer.astype(jnp.float32)
    normed = (
        widened
        * lax.rsqrt(jnp.mean(widened * widened, axis=-1, keepdims=True) + eps)
        * feedforward_norm_gain
    ).astype(jnp.bfloat16)
    gate_full, up_full = (
        lax.all_gather(gate_weight, "sp", axis=0, tiled=True),
        lax.all_gather(up_weight, "sp", axis=0, tiled=True),
    )
    down_full = lax.all_gather(down_weight, "sp", axis=1, tiled=True)
    row_piece = lax.all_gather(normed, "tp", axis=0, tiled=True)
    gate_part = jnp.dot(row_piece, gate_full, preferred_element_type=jnp.float32)
    up_part = jnp.dot(row_piece, up_full, preferred_element_type=jnp.float32)
    hidden = (jax.nn.silu(gate_part) * up_part).astype(jnp.bfloat16)
    rows_here = hidden
    ffn_sum = lax.psum_scatter(
        jnp.dot(rows_here, down_full, preferred_element_type=jnp.float32).astype(jnp.bfloat16),
        "tp",
        scatter_dimension=0,
        tiled=True,
    ).astype(jnp.float32)
    finished = (after_mixer.astype(jnp.float32) + 0.5 * ffn_sum).astype(jnp.bfloat16)
    return lax.all_gather(finished, "tp", axis=0, tiled=True)


def solution(mesh):
    return jax.shard_map(
        local,
        mesh=mesh,
        in_specs=(
            P("sp", None),
            P("sp", "tp"),
            P("sp", "tp"),
            P("sp", "tp"),
            P("sp", "tp"),
            P("tp"),
            P("sp", "tp"),
            P(),
            P("tp", None),
            P(),
            P("sp", "tp"),
            P("sp", "tp"),
            P("tp", "sp"),
        ),
        out_specs=P("sp", None),
        check_vma=False,
    )
```
